32 devices in a mesh: sp: 4 (over y, x), tp: 8 (over z, core).
Axes of the slice: x: 2, y: 2, z: 4, core: 2. Of those that a mesh axis runs over, the one named last changes fastest.
Arguments:
- tokens: bfloat16 [8, 1536, 2048], P('tp', 'sp'), may hold values from -12 to 12
- norm_gain: float32 [2, 2048], replicated, may hold values from 0.1 to 1.9
- in_weight: bfloat16 [2, 2048, 512], P(None, 'sp', 'tp'), may hold values from -0.125 to 0.125
- down_weight: bfloat16 [2, 512, 2048], P(None, 'sp', 'tp'), may hold values from -0.25 to 0.25
- pool_gain: float32 [2, 512], replicated, may hold values from 0.1 to 1.9
Outputs:
- mixed: bfloat16 [8, 1536, 2048], P('tp', 'sp')
The draws below stay inside these ranges and needn't reach their ends.
All inputs are finite; a program needn't handle non-finite values.
Results may differ from the reference program's by a relative error of at most 0.0061.
Values may be sent and summed in bfloat16 or wider, within the bound.
A program may use at most 64 MiB of HBM per device.

```python
import math
import jax
import jax.numpy as jnp
from jax import lax

D = 2048
P_SIZE = 512
GROUP = 64
LAYERS = 2
TOKENS = 1536
SEQS = 8


def draw_tokens(key, part):
    scale_key, value_key = jax.random.split(jax.random.fold_in(key, 11))
    groups = D // GROUP
    scales = jnp.exp(jax.random.uniform(scale_key, (groups,), jnp.float32, math.log(0.3), math.log(3.0)))
    values = jnp.clip(jax.random.normal(value_key, (SEQS, TOKENS, D), jnp.float32), -4.0, 4.0)
    return (values * jnp.repeat(scales, GROUP)[None, None, :]).astype(jnp.bfloat16)


def levels(rng, extent, shards, low, high):
    def one(dim, blocks):
        draws = jax.random.uniform(jax.random.fold_in(jax.random.fold_in(rng, 6), dim), (blocks,), jnp.float32, low / len(shards), high / len(shards))
        return jnp.repeat(jnp.exp(draws), extent[dim] // blocks).reshape((-1,) + (1,) * (len(extent) - dim - 1))

    level = one(*shards[0])
    for cut in shards[1:]:
        level = level * one(*cut)
    return level


def centred(key, dims, deviation, bound, cuts=(), held_as=jnp.bfloat16):
    drawn = deviation * jax.random.normal(key, dims, jnp.float32)
    if cuts:
        drawn = drawn * levels(key, dims, cuts, -0.22, 0.18)
    return jnp.clip(drawn, -bound, bound).astype(held_as)


def setup_inputs(seed: int = 0) -> dict:
    keys = jax.random.split(jax.random.key(seed), 6)
    tokens = draw_tokens(jax.random.fold_in(keys[5], 71), 0)
    norm_gain = jnp.clip(1.0 + 0.18 * jax.random.normal(keys[1], (LAYERS, D), jnp.float32), 0.1, 1.9)
    in_weight = centred(keys[2], (LAYERS, D, P_SIZE), D ** -0.5, 0.125, ((1, 4), (2, 8)))
    down_weight = centred(keys[3], (LAYERS, P_SIZE, D), P_SIZE ** -0.5, 0.25, ((1, 4), (2, 8)))
    pool_gain = jnp.clip(1.0 + 0.18 * jax.random.normal(keys[4], (LAYERS, P_SIZE), jnp.float32), 0.1, 1.9)
    return {"tokens": tokens, "norm_gain": norm_gain, "in_weight": in_weight, "down_weight": down_weight, "pool_gain": pool_gain}


EPS = 1e-06
WINDOWS = (2, 4, 8, 16)

def pool_rows(extended, first_pos, channel):
    sum_two = extended[1:] + extended[:-1]
    sum_four = sum_two[2:] + sum_two[:-2]
    sum_eight = sum_four[4:] + sum_four[:-4]
    sum_sixteen = sum_eight[8:] + sum_eight[:-8]
    count = extended.shape[0] - 15
    sums = (sum_two[-count:], sum_four[-count:], sum_eight[-count:], sum_sixteen[-count:])
    position = (first_pos + lax.iota(jnp.int32, count) + 1).astype(jnp.float32)
    which_one = channel // GROUP % 4
    result = jnp.zeros((count, extended.shape[1]), jnp.float32)
    for index, window in enumerate(WINDOWS):
        average = sums[index] / jnp.minimum(position, float(window))[:, None]
        result = jnp.where(which_one[None, :] == index, average, result)
    return result - extended[15:]

def reference(tokens, norm_gain, in_weight, down_weight, pool_gain):
    channel = lax.iota(jnp.int32, P_SIZE)

    def one_sequence(stream):
        for layer_index in range(LAYERS):
            residual = stream.astype(jnp.float32)
            inverse_rms = lax.rsqrt(lax.optimization_barrier(jnp.mean(residual * residual, axis=1, keepdims=True)) + EPS)
            normed = (residual * inverse_rms * norm_gain[layer_index]).astype(jnp.bfloat16)
            pool_in = jnp.dot(normed, in_weight[layer_index], preferred_element_type=jnp.float32).astype(jnp.bfloat16)
            extended = jnp.pad(pool_in.astype(jnp.float32), ((15, 0), (0, 0)))
            trailing = pool_rows(extended, jnp.int32(0), channel)
            pooled = (trailing * pool_gain[layer_index]).astype(jnp.bfloat16)
            down = jnp.dot(pooled, down_weight[layer_index], preferred_element_type=jnp.float32)
            stream = (residual + down).astype(jnp.bfloat16)
        return stream
    return lax.map(one_sequence, tokens)
```

```python
import functools
import math

import jax
import jax.numpy as jnp
from jax import lax
from jax.experimental import pallas as pl
from jax.experimental.pallas import tpu as pltpu
from jax.sharding import PartitionSpec as P

GROUP = 64


EPS = 1e-06
WINDOWS = (2, 4, 8, 16)


def from_behind(block, axis, distance):
    devices = range(lax.axis_size(axis))
    route = [(i - distance, i) for i in devices if i - distance in devices]
    return lax.ppermute(block, axis, route)


def pool_rows(extended, first_pos, channel):
    sum_two = extended[1:] + extended[:-1]
    sum_four = sum_two[2:] + sum_two[:-2]
    sum_eight = sum_four[4:] + sum_four[:-4]
    sum_sixteen = sum_eight[8:] + sum_eight[:-8]
    count = extended.shape[0] - 15
    sums = (sum_two[-count:], sum_four[-count:], sum_eight[-count:], sum_sixteen)
    position = (first_pos + lax.iota(jnp.int32, count) + 1).astype(jnp.float32)
    which_one = channel // GROUP % 4
    result = jnp.zeros((count, extended.shape[1]), jnp.float32)
    for index, window in enumerate(WINDOWS):
        average = sums[index] / jnp.minimum(position, float(window))[:, None]
        result = jnp.where(which_one[None, :] == index, average, result)
    return result - extended[15:]


def local(tokens, norm_gain, in_weight, down_weight, pool_gain):
    stream = tokens[0]
    tok_rows = stream.shape[0]
    pool_cols = pool_gain.shape[1]
    first_pos = lax.axis_index("sp") * tok_rows
    channel = lax.iota(jnp.int32, pool_cols)
    for layer_index in range(in_weight.shape[0]):
        residual = stream.astype(jnp.float32)
        inverse_rms = lax.rsqrt(jnp.mean(residual * residual, axis=1, keepdims=True) + EPS)
        normed = (residual * inverse_rms * norm_gain[layer_index]).astype(jnp.bfloat16)
        layer_in, layer_down = (
            lax.all_gather(in_weight[layer_index], "tp", axis=1, tiled=True),
            lax.all_gather(down_weight[layer_index], "tp", axis=1, tiled=True),
        )
        pool_acc = jnp.dot(
            normed,
            lax.all_gather(layer_in, "sp", axis=0, tiled=True),
            preferred_element_type=jnp.float32,
        )
        pool_in = pool_acc.astype(jnp.bfloat16)
        before = from_behind(pool_in[tok_rows - 15 :], "sp", 1)
        extended = jnp.concatenate([before, pool_in], axis=0).astype(jnp.float32)
        trailing = pool_rows(extended, first_pos, channel)
        pooled = (trailing * pool_gain[layer_index]).astype(jnp.bfloat16)
        down = jnp.dot(
            pooled,
            lax.all_gather(layer_down, "sp", axis=0, tiled=True),
            preferred_element_type=jnp.float32,
        )
        stream = (residual + down).astype(jnp.bfloat16)
    return stream[None]


UNITS = ((False, 0, False), (True, 0, False), (True, 1, False), (False, 1, True))
MESH = pl.DeviceIdType.MESH


def mixer_kernel(
    n_z, rows_sp,
    tok_hbm, norm_gain, in_hbm, down_hbm, pool_gain, out,
    w_in, w_down, normed, pool, pooled, halo,
    recv_sem, z_sem, a_sem, b_sem, d_sem, d_recv, h_send, h_recv, local_sem,
):
    n_s = 4
    tok = out.at[0]
    s, t = lax.axis_index("sp"), lax.axis_index("tp")
    z, c = t // 2, t % 2
    y, x = s // 2, s % 2
    s_x, s_y = y * 2 + (1 - x), (1 - y) * 2 + x
    s_a, s_b, s_d = s_x + c * (s_y - s_x), s_y + c * (s_x - s_y), 3 - s
    partner = z * 2 + (1 - c)
    in_cols, in_rows = in_hbm.shape[1:]
    d_rows, d_cols = down_hbm.shape[1:]
    n_tok, width = tok.shape
    p_size = pool.shape[1]

    def unit(u, us, uz):
        is_in, layer, _ = UNITS[u]
        if is_in:
            col = pl.multiple_of((uz * 2 + c) * in_cols, in_cols)
            return w_in.at[layer, pl.ds(col, in_cols), pl.ds(pl.multiple_of(us * in_rows, in_rows), in_rows)]
        row = pl.multiple_of(us * d_rows, d_rows)
        return w_down.at[layer, pl.ds(row, d_rows), pl.ds(pl.multiple_of((uz * 2 + c) * d_cols, d_cols), d_cols)]

    def many(u, k):
        is_in, layer, _ = UNITS[u]
        if is_in:
            return w_in.at[layer, pl.ds(0, in_cols * k), pl.ds(0, in_rows * n_z)]
        return w_down.at[layer, pl.ds(0, d_rows // 2 * k), :]

    def few(u, k):
        is_in, layer, _ = UNITS[u]
        if is_in:
            return w_in.at[layer, pl.ds(0, in_cols * k), pl.ds(0, in_rows)]
        return w_down.at[layer, pl.ds(0, d_rows * k), pl.ds(0, d_cols)]

    def number(u, us, uz):
        return u * (n_s * n_z) + us * n_z + uz

    def to(u, us, uz, send, device_s, device_t):
        ref = unit(u, us, uz)
        return pltpu.make_async_remote_copy(
            ref, ref, send, recv_sem.at[number(u, us, uz)],
            device_id=(device_s, device_t), device_id_type=MESH)

    def to_up(u, us, uz):
        return to(u, us, uz, z_sem.at[((u * 2) * n_s + us) * n_z + uz], s, t + 2)

    def to_down(u, us, uz):
        return to(u, us, uz, z_sem.at[((u * 2 + 1) * n_s + us) * n_z + uz], s, t - 2)

    def to_a(u, uz):
        return to(u, s, uz, a_sem.at[u], s_a, t)

    def to_b(u, us, uz):
        return to(u, us, uz, b_sem.at[u], s_b, t)

    def to_partner(u, us, uz):
        ref = unit(u, us, uz)
        return pltpu.make_async_remote_copy(
            ref, ref, d_sem.at[u], d_recv.at[u], device_id=(s, partner), device_id_type=MESH)

    def arrive(u, us, uz):
        ref = unit(u, us, uz)
        pltpu.make_async_copy(ref, ref, recv_sem.at[number(u, us, uz)]).wait()

    def up(u, us, uz, finish=False):
        @pl.when(z < n_z - 1)
        def _():
            to_up(u, us, uz).wait_send() if finish else to_up(u, us, uz).start()

    def down(u, us, uz, finish=False):
        @pl.when(z > 0)
        def _():
            to_down(u, us, uz).wait_send() if finish else to_down(u, us, uz).start()

    def own(u):
        placed[u].wait()
        up(u, s, z)
        down(u, s, z)
        to_b(u, s, z).start()
        to_a(u, z).start()
        to_partner(u, s, z).start()

    def at_distance(d, body):
        if d == 0:
            body(z, True)
            return

        @pl.when(z - d >= 0)
        def _():
            body(z - d, True)

        @pl.when(z + d < n_z)
        def _():
            body(z + d, False)

    def places(u):
        return (s, s_a, s_b, s_d) if UNITS[u][2] else (s,)

    def along_z(u, d):
        def body(uz, from_below):
            for us in places(u):
                arrive(u, us, uz)
                up(u, us, uz) if from_below else down(u, us, uz)
                if not UNITS[u][2]:
                    to_b(u, us, uz).start()
                    to_a(u, uz).start()
                to_partner(u, us, uz).start()
        at_distance(d, body)

    def along_a(u, d):
        def body(uz, _):
            arrive(u, s_a, uz)
            to_b(u, s_a, uz).start()
            if UNITS[u][2]:
                up(u, s_a, uz)
                down(u, s_a, uz)
            to_partner(u, s_a, uz).start()
        at_distance(d, body)

    def along_b(u, d):
        def body(uz, _):
            for us in (s_b, s_d):
                arrive(u, us, uz)
                if UNITS[u][2]:
                    up(u, us, uz)
                    down(u, us, uz)
                to_partner(u, us, uz).start()
        at_distance(d, body)

    def ready(u):
        pltpu.make_async_copy(many(u, 4), many(u, 4), d_recv.at[u]).wait()

    def local_copy(src, dst, index):
        return pltpu.make_async_copy(src, dst, local_sem.at[index])

    barrier = pltpu.get_barrier_semaphore()

    def greet(device_s, device_t):
        pl.semaphore_signal(barrier, inc=1, device_id=(device_s, device_t), device_id_type=MESH)

    greet(s, partner)
    greet(s_x, t)
    greet(s_y, t)
    for cond, ds, dt in ((z > 0, s, t - 2), (z < n_z - 1, s, t + 2), (s > 0, s - 1, t), (s < n_s - 1, s + 1, t)):
        @pl.when(cond)
        def _():
            greet(ds, dt)

    placed = [
        local_copy((in_hbm if is_in else down_hbm).at[l], unit(u, s, z), u) for u, (is_in, l, _) in enumerate(UNITS)
    ]
    tok_in = local_copy(tok_hbm.at[0], tok, 4)
    for copy in placed:
        copy.start()
    tok_in.start()
    met = 3
    for cond in (z > 0, z < n_z - 1, s > 0, s < n_s - 1):
        met = met + jnp.where(cond, 1, 0)
    pl.semaphore_wait(barrier, met)

    def norm(layer):
        step = 32

        def body(i, carry):
            at = pl.ds(pl.multiple_of(i * step, step), step)
            value = tok[at, :].astype(jnp.float32)
            inverse = lax.rsqrt(jnp.mean(value * value, axis=1, keepdims=True) + EPS)
            normed[at, :] = (value * inverse * norm_gain[layer : layer + 1, :]).astype(jnp.bfloat16)
            return carry
        lax.fori_loop(0, n_tok // step, body, 0)

    def project_in(layer):
        tile = 256
        for j in range(p_size // tile):
            cols = pl.ds(j * tile, tile)
            pool[:, cols] = lax.dot_general(
                normed[...], w_in[layer, cols, :], (((1,), (1,)), ((), ())),
                preferred_element_type=jnp.float32).astype(jnp.bfloat16)

    def halo_copy(layer):
        return pltpu.make_async_remote_copy(
            pool.at[pl.ds(n_tok - 16, 16), :], halo.at[layer], h_send.at[layer], h_recv.at[layer],
            device_id=(s + 1, t), device_id_type=MESH)

    def send_halo(layer):
        @pl.when(s < n_s - 1)
        def _():
            halo_copy(layer).start()

    def pool_all(layer):
        lanes, head = 128, 128
        for start, size in ((head, n_tok - head), (0, head)):
            if start == 0:
                @pl.when(s > 0)
                def _():
                    halo_copy(layer).wait_recv()

                @pl.when(s == 0)
                def _():
                    halo[layer] = jnp.zeros(halo.shape[1:], halo.dtype)

            lane = lax.broadcasted_iota(jnp.int32, (size, lanes), 1)
            position = (s * n_tok + lax.broadcasted_iota(jnp.int32, (size, lanes), 0) + 1).astype(jnp.float32)
            for j in range(p_size // lanes):
                cols = pl.ds(j * lanes, lanes)
                if start == 0:
                    value = jnp.concatenate([halo[layer, :, cols], pool[:size, cols]], axis=0)
                else:
                    value = pool[start - 16 :, cols]
                value = value.astype(jnp.float32)
                sums, total, reach = {}, value, 1
                for window in WINDOWS:
                    total = total + pltpu.roll(total, reach, 0)
                    sums[window] = total
                    reach *= 2
                result = None
                for g in range(lanes // GROUP):
                    window = WINDOWS[(j * lanes // GROUP + g) % 4]
                    if start == 0:
                        average = sums[window][16:] / jnp.minimum(position, float(window))
                    else:
                        average = sums[window][16:] * (1.0 / window)
                    result = average if result is None else jnp.where(lane < g * GROUP, result, average)
                result = (result - value[16:]) * pool_gain[layer : layer + 1, cols]
                pooled[start : start + size, cols] = result.astype(jnp.bfloat16)

        @pl.when(s < n_s - 1)
        def _():
            halo_copy(layer).wait_send()

    def project_down(layer, last):
        tile = 256

        def body(j, carry):
            cols = pl.ds(pl.multiple_of(j * tile, tile), tile)
            down = jnp.dot(pooled[...], w_down[layer, :, cols], preferred_element_type=jnp.float32)
            tok[:, cols] = (tok[:, cols].astype(jnp.float32) + down).astype(jnp.bfloat16)
            return carry
        lax.fori_loop(0, width // tile, body, 0)

    far = range(n_z)
    own(0)
    own(1)
    own(2)
    own(3)
    tok_in.wait()
    along_z(0, 1)
    along_z(1, 1)
    norm(0)
    along_a(0, 0)
    along_a(1, 0)
    along_a(3, 0)
    along_b(3, 0)
    along_z(0, 2)
    along_z(1, 2)
    along_a(0, 1)
    along_a(1, 1)
    along_z(2, 1)
    along_z(0, 3)
    along_z(1, 3)
    along_a(0, 2)
    along_a(1, 2)
    along_a(2, 0)
    along_z(3, 1)
    along_a(0, 3)
    along_a(1, 3)
    along_z(2, 2)
    along_a(2, 1)
    for d in far:
        along_b(0, d)
    for d in far:
        along_b(1, d)
    ready(0)
    ready(1)
    project_in(0)
    send_halo(0)
    along_z(2, 3)
    along_a(2, 2)
    along_z(3, 2)
    pool_all(0)
    along_a(2, 3)
    project_down(0, False)
    norm(1)
    along_z(3, 3)
    for d in far:
        along_b(2, d)
    ready(2)
    project_in(1)
    send_halo(1)
    pool_all(1)
    ready(3)
    project_down(1, True)

    for u, (_, _, z_last) in enumerate(UNITS):
        for ref, sem in (
            (few(u, 1) if z_last else many(u, 1), a_sem),
            (few(u, 2) if z_last else many(u, 2), b_sem),
            (many(u, 4), d_sem),
        ):
            pltpu.make_async_copy(ref, ref, sem.at[u]).wait()

        def body(uz, from_below):
            for us in places(u):
                up(u, us, uz, True) if from_below else down(u, us, uz, True)

        for us in places(u):
            up(u, us, z, True)
            down(u, us, z, True)
        for d in range(1, n_z):
            at_distance(d, body)


def fused(n_z, tokens, norm_gain, in_weight, down_weight, pool_gain):
    n_tok, width = tokens.shape[1:]
    p_size = pool_gain.shape[1]
    n_u = len(UNITS)
    any_spec, vmem = pl.BlockSpec(memory_space=pltpu.HBM), pl.BlockSpec(memory_space=pltpu.VMEM)
    dma = pltpu.SemaphoreType.DMA
    bf16 = jnp.bfloat16
    return pl.pallas_call(
        functools.partial(mixer_kernel, n_z, 4),
        out_shape=pltpu.VMEM(tokens.shape, tokens.dtype),
        in_specs=[any_spec, vmem, any_spec, any_spec, vmem],
        out_specs=vmem,
        scratch_shapes=[
            pltpu.VMEM((2, p_size, width), bf16),
            pltpu.VMEM((2, p_size, width), bf16),
            pltpu.VMEM((n_tok, width), bf16),
            pltpu.VMEM((n_tok, p_size), bf16),
            pltpu.VMEM((n_tok, p_size), bf16),
            pltpu.VMEM((2, 16, p_size), bf16),
            dma((n_u * 4 * n_z,)),
            dma((n_u * 2 * 4 * n_z,)),
            dma((n_u,)),
            dma((n_u,)),
            dma((n_u,)),
            dma((n_u,)),
            dma((2,)),
            dma((2,)),
            dma((5,)),
        ],
        compiler_params=pltpu.CompilerParams(
            collective_id=0, has_side_effects=True, vmem_limit_bytes=67_043_328 - 2 * n_tok * width),
    )(tokens, norm_gain, jnp.swapaxes(in_weight, 1, 2), down_weight, pool_gain)


def fits(n_sp, n_tp, tokens, in_weight, down_weight):
    n_tok, width = tokens.shape[1:]
    layers, in_rows, in_cols = in_weight.shape
    d_rows, d_cols = down_weight.shape[1:]
    return (
        n_sp == 4 and n_tp % 2 == 0 and layers == 2 and tokens.shape[0] == 1
        and in_cols % 32 == 0 and d_cols % 128 == 0 and d_rows % 32 == 0 and in_rows % 128 == 0
        and n_tp * in_cols == 4 * d_rows
        and n_tok % 128 == 0 and n_tok > 128 and width % 256 == 0 and width * n_tok <= 2**20
    )


def solution(mesh):
    n_sp, n_tp = mesh.shape["sp"], mesh.shape["tp"]
    in_specs = (P("tp", "sp", None), P(), P(None, "sp", "tp"), P(None, "sp", "tp"), P())
    out_specs = P("tp", "sp", None)

    def per_device(tokens, norm_gain, in_weight, down_weight, pool_gain):
        if fits(n_sp, n_tp, tokens, in_weight, down_weight):
            return fused(n_tp // 2, tokens, norm_gain, in_weight, down_weight, pool_gain)
        return local(tokens, norm_gain, in_weight, down_weight, pool_gain)

    return jax.shard_map(per_device, mesh=mesh, in_specs=in_specs, out_specs=out_specs, check_vma=False)
```
